32 devices in a mesh: grp: 2 (over y), dp: 2 (over x), kv: 4 (over z), tp: 2 (over core).
Axes of the slice: x: 2, y: 2, z: 4, core: 2. Of those that a mesh axis runs over, the one named last changes fastest.
Arguments:
- residual_input: bfloat16 [128, 4096], P(('grp', 'dp', 'tp'), 'kv'), parts along dimension 0, may hold values from -6 to 6
- incoming_state: float32 [128, 16, 64, 128], P(('grp', 'kv'), ('dp', 'tp')), parts along dimension 0, may hold values from -4 to 4
- extra_log_decay: float32 [128, 1024], P(('grp', 'kv'), ('dp', 'tp')), parts along dimension 0, may hold values from -0.7 to 0
- leading_norm_gain: float32 [4096], P('kv'), may hold values from 0.1 to 1.9
- leading_gate_weight: bfloat16 [4096, 11264], P('kv', ('dp', 'tp')), may hold values from -0.09375 to 0.09375
- leading_up_weight: bfloat16 [4096, 11264], P('kv', ('dp', 'tp')), may hold values from -0.09375 to 0.09375
- leading_down_weight: bfloat16 [11264, 4096], P(('dp', 'tp'), 'kv'), may hold values from -0.0546875 to 0.0546875
- attention_norm_gain: float32 [4096], P('kv'), may hold values from 0.1 to 1.9
- query_projector: bfloat16 [4096, 1024], P('kv', ('dp', 'tp')), may hold values from -0.09375 to 0.09375
- key_projector: bfloat16 [4096, 1024], P('kv', ('dp', 'tp')), may hold values from -0.09375 to 0.09375
- value_projector: bfloat16 [4096, 2048], P('kv', ('dp', 'tp')), may hold values from -0.09375 to 0.09375
- output_gate_weight: bfloat16 [4096, 2048], P('kv', ('dp', 'tp')), may hold values from -0.09375 to 0.09375
- forget_weight: bfloat16 [4096, 1024], P('kv', ('dp', 'tp')), may hold values from -0.75 to 0.75
- head_norm_gain: float32 [128], replicated, may hold values from 0.1 to 1.9
- output_projector: bfloat16 [2048, 4096], P(('dp', 'tp'), 'kv'), may hold values from -0.125 to 0.125
- trailing_norm_gain: float32 [4096], P('kv'), may hold values from 0.1 to 1.9
- trailing_gate_weight: bfloat16 [4096, 11264], P('kv', ('dp', 'tp')), may hold values from -0.09375 to 0.09375
- trailing_up_weight: bfloat16 [4096, 11264], P('kv', ('dp', 'tp')), may hold values from -0.09375 to 0.09375
- trailing_down_weight: bfloat16 [11264, 4096], P(('dp', 'tp'), 'kv'), may hold values from -0.0546875 to 0.0546875
Outputs:
- result: bfloat16 [128, 4096], P(('grp', 'dp', 'tp'), 'kv'), parts along dimension 0
- new_state: float32 [128, 16, 64, 128], P(('grp', 'kv'), ('dp', 'tp')), parts along dimension 0
The draws below stay inside these ranges and needn't reach their ends.
There are 2 independent parts, one for each index of `grp`. The reference program is written for one: setup_inputs(seed, part) draws one part's arguments, and reference() takes and returns one part's arrays. A program takes and returns all parts, laid end to end along the dimension named above; an argument that names none is the same for every part. Nothing has to cross between parts.
All inputs are finite; a program needn't handle non-finite values.
Results may differ from the reference program's by a relative error of at most 0.0095.
Values may be sent and summed in bfloat16 or wider, within the bound.
A program may use at most 128 MiB of HBM per device.

```python
import jax
import jax.numpy as jnp
from jax import lax

D = 4096
FF = 11264
HEAD_COUNT = 16
KEY_CHANNELS = 64
VALUE_DIM = 128
BATCH_SIZE = 64


def shard_levels(stream_key, shape, split, low, largest):
    level, own = 1.0, jax.random.fold_in(stream_key, 6)
    for axis_at, parts in split:
        steps = jnp.exp(jax.random.uniform(jax.random.fold_in(own, axis_at), (parts,), jnp.float32, low / len(split), largest / len(split)))
        level = level * jnp.repeat(steps, shape[axis_at] // parts).reshape([-1 if axis == axis_at else 1 for axis in range(len(shape))])
    return level


def bell_draw(key, extent, spread, limit, cuts=(), held_as=jnp.bfloat16):
    factor_of = shard_levels(key, extent, cuts, -0.22, 0.18) if cuts else 1.0
    values = jax.random.normal(key, extent, jnp.float32) * spread * factor_of
    return jnp.minimum(jnp.maximum(values, -limit), limit).astype(held_as)


def setup_inputs(seed: int = 0, part: int = 0) -> dict:
    splits = jax.random.split(jax.random.key(seed), 20)
    own_keys = jax.random.split(jax.random.fold_in(splits[19], part), 20)
    return {
        "residual_input": bell_draw(own_keys[0], (BATCH_SIZE, D), 1.0, 6.0, ((0, 4), (1, 4))),
        "incoming_state": bell_draw(own_keys[1], (BATCH_SIZE, HEAD_COUNT, KEY_CHANNELS, VALUE_DIM), 0.5, 4.0, ((0, 4), (1, 4)), jnp.float32),
        "extra_log_decay": jnp.clip(-0.7 + 0.7 * jax.random.uniform(own_keys[2], (BATCH_SIZE, HEAD_COUNT * KEY_CHANNELS), jnp.float32) ** shard_levels(own_keys[2], (BATCH_SIZE, HEAD_COUNT * KEY_CHANNELS), ((0, 4), (1, 4)), -0.2, 0.2), -0.7, 0.0),
        "leading_norm_gain": jnp.clip(1.0 + 0.18 * jax.random.normal(splits[3], (D,), jnp.float32), 0.1, 1.9),
        "leading_gate_weight": bell_draw(splits[4], (D, FF), D ** -0.5, 0.09375, ((0, 4), (1, 4))),
        "leading_up_weight": bell_draw(splits[5], (D, FF), D ** -0.5, 0.09375, ((0, 4), (1, 4))),
        "leading_down_weight": bell_draw(splits[6], (FF, D), FF ** -0.5, 0.0546875, ((0, 4), (1, 4))),
        "attention_norm_gain": jnp.clip(1.0 + 0.18 * jax.random.normal(splits[7], (D,), jnp.float32), 0.1, 1.9),
        "query_projector": bell_draw(splits[8], (D, HEAD_COUNT * KEY_CHANNELS), D ** -0.5, 0.09375, ((0, 4), (1, 4))),
        "key_projector": bell_draw(splits[9], (D, HEAD_COUNT * KEY_CHANNELS), D ** -0.5, 0.09375, ((0, 4), (1, 4))),
        "value_projector": bell_draw(splits[10], (D, HEAD_COUNT * VALUE_DIM), D ** -0.5, 0.09375, ((0, 4), (1, 4))),
        "output_gate_weight": bell_draw(splits[11], (D, HEAD_COUNT * VALUE_DIM), D ** -0.5, 0.09375, ((0, 4), (1, 4))),
        "forget_weight": bell_draw(splits[12], (D, HEAD_COUNT * KEY_CHANNELS), (max(D // 64, 1)) ** -0.5, 0.75, ((0, 4), (1, 4))),
        "head_norm_gain": jnp.clip(1.0 + 0.18 * jax.random.normal(splits[13], (VALUE_DIM,), jnp.float32), 0.1, 1.9),
        "output_projector": bell_draw(splits[14], (HEAD_COUNT * VALUE_DIM, D), (HEAD_COUNT * VALUE_DIM) ** -0.5, 0.125, ((0, 4), (1, 4))),
        "trailing_norm_gain": jnp.clip(1.0 + 0.18 * jax.random.normal(splits[15], (D,), jnp.float32), 0.1, 1.9),
        "trailing_gate_weight": bell_draw(splits[16], (D, FF), D ** -0.5, 0.09375, ((0, 4), (1, 4))),
        "trailing_up_weight": bell_draw(splits[17], (D, FF), D ** -0.5, 0.09375, ((0, 4), (1, 4))),
        "trailing_down_weight": bell_draw(splits[18], (FF, D), FF ** -0.5, 0.0546875, ((0, 4), (1, 4))),
    }


epsilon = 1e-06

def row_scale(row_block):
    widened = row_block.astype(jnp.float32)
    return lax.rsqrt(lax.optimization_barrier(jnp.sum(widened * widened, axis=1, keepdims=True)) / D + epsilon)

def channel_mixer(row_block, norm_gain, gate_matrix, up_matrix, down_matrix):
    decay_factor = row_scale(row_block)
    scaled = (row_block.astype(jnp.float32) * norm_gain).astype(jnp.bfloat16)
    gate_sum = decay_factor * jnp.dot(scaled, gate_matrix, preferred_element_type=jnp.float32)
    up_sum = decay_factor * jnp.dot(scaled, up_matrix, preferred_element_type=jnp.float32)
    hidden = (jax.nn.silu(gate_sum) * up_sum).astype(jnp.bfloat16)
    return jnp.dot(hidden, down_matrix, preferred_element_type=jnp.float32)

def reference(residual_input, incoming_state, extra_log_decay, leading_norm_gain, leading_gate_weight, leading_up_weight, leading_down_weight, attention_norm_gain, query_projector, key_projector, value_projector, output_gate_weight, forget_weight, head_norm_gain, output_projector, trailing_norm_gain, trailing_gate_weight, trailing_up_weight, trailing_down_weight):
    after_first = (residual_input.astype(jnp.float32) + 0.5 * channel_mixer(residual_input, leading_norm_gain, leading_gate_weight, leading_up_weight, leading_down_weight)).astype(jnp.bfloat16)
    decay_factor = row_scale(after_first)
    scaled = (after_first.astype(jnp.float32) * attention_norm_gain).astype(jnp.bfloat16)

    def apply_projection(matrix):
        return decay_factor * jnp.dot(scaled, matrix, preferred_element_type=jnp.float32)
    queries = apply_projection(query_projector).reshape(BATCH_SIZE, HEAD_COUNT, KEY_CHANNELS) * KEY_CHANNELS ** (-0.5)
    key_rows = apply_projection(key_projector).reshape(BATCH_SIZE, HEAD_COUNT, KEY_CHANNELS)
    value_rows = apply_projection(value_projector).reshape(BATCH_SIZE, HEAD_COUNT, VALUE_DIM)
    gate_rows = apply_projection(output_gate_weight).reshape(BATCH_SIZE, HEAD_COUNT, VALUE_DIM)
    decay_logarithm = (jax.nn.log_sigmoid(apply_projection(forget_weight)) / 16.0 + extra_log_decay).reshape(BATCH_SIZE, HEAD_COUNT, KEY_CHANNELS)
    new_state = jnp.exp(decay_logarithm)[..., None] * incoming_state + key_rows[..., None] * value_rows[:, :, None, :]
    read_out = jnp.einsum('bhk,bhkv->bhv', queries, new_state, precision=lax.Precision.HIGHEST)
    normed = read_out * lax.rsqrt(lax.optimization_barrier(jnp.mean(read_out * read_out, axis=-1, keepdims=True)) + epsilon)
    head_rows = (normed * head_norm_gain * jax.nn.silu(gate_rows)).astype(jnp.bfloat16).reshape(BATCH_SIZE, HEAD_COUNT * VALUE_DIM)
    second = (after_first.astype(jnp.float32) + jnp.dot(head_rows, output_projector, preferred_element_type=jnp.float32)).astype(jnp.bfloat16)
    result = (second.astype(jnp.float32) + 0.5 * channel_mixer(second, trailing_norm_gain, trailing_gate_weight, trailing_up_weight, trailing_down_weight)).astype(jnp.bfloat16)
    return (result, new_state)
```

```python
import functools

import jax
import jax.numpy as jnp
from jax import lax
from jax.experimental import pallas as pl
from jax.experimental.pallas import tpu as pltpu
from jax.sharding import PartitionSpec as P

KEY_CHANNELS = 64
VALUE_DIM = 128
LANES = 128
epsilon = 1e-06
MESH = pl.DeviceIdType.MESH
F32 = jnp.float32
BF16 = jnp.bfloat16
CHUNKS = 4
PAIRS = 4
RELAYED_SUMS = (0, 1)
RELAYED_HIDDEN = (0, 1)


def spans(width, count):
    if width % LANES:
        return [(0, width)]
    tile = 2 * LANES if width % (2 * LANES) == 0 else LANES
    tiles = width // tile
    count = min(count, tiles)
    cuts = [tile * ((tiles * i + count - 1) // count) for i in range(count + 1)]
    return list(zip(cuts[:-1], cuts[1:]))


def padded(width):
    return -(-width // LANES) * LANES


def silu(x):
    return x * jax.nn.sigmoid(x)


def kernel(dims, names, *refs):
    R, K, TP, D, B, d, F, W, V, heads = dims
    mr, mk, DP = B // R, B // K, R // TP
    ref = dict(zip(names, refs))
    dp_i, tp_i, k = lax.axis_index("dp"), lax.axis_index("tp"), lax.axis_index("kv")
    r = dp_i * TP + tp_i
    Wp = padded(W)
    kv_order = sorted(range(1, K), key=lambda o: abs(2 * o - K))
    counter = {"send": 0, "recv": 0, "local": 0}
    pending = []
    inner_pending, outer_pending = [], []
    paired = K == PAIRS
    if paired:
        side = k // 2
        partner = k + 1 - 2 * lax.rem(k, 2)
        near, far = 2 - side, 3 * (1 - side)
        across = 2 * (1 - side)
        inner = lax.rem(k + 1, K) // 2 == 1
        outer = jnp.logical_not(inner)
        slot = jnp.where(inner, 1, 2)

    def row_peer(o):
        t = lax.rem(r + o, R)
        return t, {"dp": t // TP, "tp": lax.rem(t, TP)}

    def kv_peer(o):
        t = lax.rem(k + o, K)
        return t, {"kv": t}

    def local(src, dst):
        i = counter["local"]
        counter["local"] += 1
        copy = pltpu.make_async_copy(src, dst, ref["local_sem"].at[i])
        copy.start()
        return copy

    def reserve(count):
        i = counter["recv"]
        counter["recv"] += count
        return i

    def described(src, dst, device, arrival, held):
        i = counter["send"]
        counter["send"] += 1
        copy = pltpu.make_async_remote_copy(
            src_ref=src,
            dst_ref=dst,
            send_sem=ref["send_sem"].at[i],
            recv_sem=ref["recv_sem"].at[arrival],
            device_id=device,
            device_id_type=MESH,
        )
        held.append(copy)
        return copy

    def remote(src, dst, device, arrival=None):
        arrival = reserve(1) if arrival is None else arrival
        copy = described(src, dst, device, arrival, pending)
        copy.start()
        return copy

    def arrived(dst, arrival):
        pltpu.make_async_remote_copy(
            src_ref=dst,
            dst_ref=dst,
            send_sem=ref["send_sem"].at[0],
            recv_sem=ref["recv_sem"].at[arrival],
            device_id={"kv": partner},
            device_id_type=MESH,
        ).wait_recv()

    own_x = local(ref["x"], ref["x_all"].at[r])
    load_g1 = local(ref["g1"], ref["g1_v"])
    fspans = spans(F, CHUNKS)

    def load_mixer(p):
        first = []
        for a, b in fspans:
            cut = (slice(None), slice(None)) if b - a == F else (slice(None), pl.ds(a, b - a))
            first.append(
                (
                    local(ref[p + "g"].at[cut], ref[p + "g_v"].at[cut]),
                    local(ref[p + "u"].at[cut], ref[p + "u_v"].at[cut]),
                )
            )
        return first, local(ref[p + "d"], ref[p + "d_v"])

    lead = load_mixer("l")
    load_attn = [local(ref[n], ref[n + "_v"]) for n in ("g2", "wq", "wk", "wf", "wv", "wg")]
    load_state = [local(ref[n], ref[n + "_v"]) for n in ("st", "eld", "hng")]
    load_out = local(ref["wo"], ref["wo_v"])
    load_g3 = local(ref["g3"], ref["g3_v"])
    trail = load_mixer("t")

    barrier = pltpu.get_barrier_semaphore()
    for o in range(1, R):
        pl.semaphore_signal(barrier, inc=1, device_id=row_peer(o)[1], device_id_type=MESH)
    for o in kv_order:
        pl.semaphore_signal(barrier, inc=1, device_id=kv_peer(o)[1], device_id_type=MESH)
    pl.semaphore_wait(barrier, R - 1 + K - 1)

    def gather_rows(src, buf):
        copies = [remote(src, buf.at[r], row_peer(o)[1]) for o in range(1, R)]
        return copies

    def wait_all(copies):
        for copy in copies:
            copy.wait_recv()

    def normalised(buf, gain):
        wide = buf[...].reshape(B, d).astype(F32)
        squares = jnp.sum(wide * wide, axis=1, keepdims=True)
        ref["scaled"][...] = (wide * gain[...]).astype(BF16)
        return jnp.broadcast_to(squares, (B, LANES)).reshape(K, mk, LANES)

    def row_scale(total):
        return lax.rsqrt(total / D + epsilon)[:, :1]

    def mixer_direct(p, buf, gain, loads):
        gu_loads, down_load = loads
        gu_send, gu_recv = ref[p + "gu_send"], ref[p + "gu_recv"]
        ss_send, ss_recv = ref[p + "ss_send"], ref[p + "ss_recv"]
        h_all = ref[p + "h_all"]
        ss_send[...] = normalised(buf, gain)
        ss_copies = []
        for o in kv_order:
            t, device = kv_peer(o)
            ss_copies.append(remote(ss_send.at[t], ss_recv.at[o - 1], device))
        gu_copies = []
        for (a, b), pair in zip(fspans, gu_loads):
            for i, part in enumerate("gu"):
                pair[i].wait()
                product = jnp.dot(
                    ref["scaled"][...], ref[p + part + "_v"][:, a:b], preferred_element_type=F32
                )
                gu_send[:, i, :, a:b] = product.astype(BF16).reshape(K, mk, b - a)
            group = []
            for o in kv_order:
                t, device = kv_peer(o)
                if b - a == F:
                    src, dst = gu_send.at[t], gu_recv.at[o - 1]
                else:
                    src = gu_send.at[t, :, :, pl.ds(a, b - a)]
                    dst = gu_recv.at[o - 1, :, :, pl.ds(a, b - a)]
                group.append(remote(src, dst, device))
            gu_copies.append(group)
        wait_all(ss_copies)
        total = ss_send[k]
        for o in kv_order:
            total = total + ss_recv[o - 1]
        scale = row_scale(total)
        h_copies = []
        for (a, b), group in zip(fspans, gu_copies):
            wait_all(group)
            gate = gu_send[k, 0, :, a:b].astype(F32)
            up = gu_send[k, 1, :, a:b].astype(F32)
            for o in kv_order:
                gate = gate + gu_recv[o - 1, 0, :, a:b].astype(F32)
                up = up + gu_recv[o - 1, 1, :, a:b].astype(F32)
            h_all[k, :, a:b] = (silu(scale * gate) * (scale * up)).astype(BF16)
            mine = h_all.at[k] if b - a == F else h_all.at[k, :, pl.ds(a, b - a)]
            h_copies.append([remote(mine, mine, kv_peer(o)[1]) for o in kv_order])
        down_load.wait()
        acc = None
        for (a, b), group in zip(fspans, h_copies):
            wait_all(group)
            part = jnp.dot(
                h_all[:, :, a:b].reshape(B, b - a),
                ref[p + "d_v"][a:b, :],
                preferred_element_type=F32,
            )
            acc = part if acc is None else acc + part
        return acc

    def part(buf, i, a, b):
        return buf.at[i] if b - a == F else buf.at[i, :, :, pl.ds(a, b - a)]

    def mixer_paired(p, buf, gain, loads):
        gu_loads, down_load = loads
        gu_f, gu_send, gu_recv = ref["gu_f"], ref[p + "gu_send"], ref[p + "gu_recv"]
        relay = ref[p + "relay"]
        ss_send, ss_recv = ref[p + "ss_send"], ref[p + "ss_recv"]
        h_all = ref[p + "h_all"]
        ss_send[...] = normalised(buf, gain)
        ss_copies = []
        for o in kv_order:
            t, device = kv_peer(o)
            ss_copies.append(remote(ss_send.at[t], ss_recv.at[o - 1], device))
        sums, relays, hiddens = [], [], []
        for c, ((a, b), pair) in enumerate(zip(fspans, gu_loads)):
            for i, name in enumerate("gu"):
                pair[i].wait()
                product = jnp.dot(
                    ref["scaled"][...], ref[p + name + "_v"][:, a:b], preferred_element_type=F32
                ).reshape(K, mk, b - a)
                gu_f[:, i, :, a:b] = product
                gu_send[:, i, :, a:b] = product.astype(BF16)
            sums.append(reserve(3))
            relays.append(reserve(1) if c in RELAYED_SUMS else None)
            if c in RELAYED_SUMS:
                cut = (pl.ds(across, 2), slice(None), slice(None), pl.ds(a, b - a))
                where = (slice(None), slice(None), slice(None), pl.ds(a, b - a))
                copy = described(
                    gu_send.at[cut], relay.at[where], {"kv": partner}, relays[c], outer_pending
                )
                pl.when(outer)(copy.start)
            else:
                for t in (far, near):
                    remote(
                        part(gu_send, t, a, b),
                        part(gu_recv, slot, a, b),
                        {"kv": t},
                        sums[c] + slot,
                    )
            remote(part(gu_send, partner, a, b), part(gu_recv, 0, a, b), {"kv": partner}, sums[c])

        relayed = []
        for c, (a, b) in enumerate(fspans):
            if c not in RELAYED_SUMS:
                continue
            onward = [
                described(
                    part(gu_send, t, a, b),
                    part(gu_recv, 1, a, b),
                    {"kv": t},
                    sums[c] + 1,
                    inner_pending,
                )
                for t in (far, near)
            ]
            relayed.append((c, a, b, onward))

        @pl.when(inner)
        def _():
            for c, a, b, onward in relayed:
                where = (slice(None), slice(None), slice(None), pl.ds(a, b - a))
                arrived(relay.at[where], relays[c])
                both = gu_f[pl.ds(across, 2), :, :, a:b] + relay[:, :, :, a:b].astype(F32)
                gu_send[pl.ds(across, 2), :, :, a:b] = both.astype(BF16)
                for copy in onward:
                    copy.start()

        wait_all(ss_copies)
        total = ss_send[k]
        for o in kv_order:
            total = total + ss_recv[o - 1]
        scale = row_scale(total)
        for c, (a, b) in enumerate(fspans):
            gate, up = gu_f[k, 0, :, a:b], gu_f[k, 1, :, a:b]
            for i in (0, 1) if c in RELAYED_SUMS else (0, 1, 2):
                arrived(part(gu_recv, i, a, b), sums[c] + i)
                gate = gate + gu_recv[i, 0, :, a:b].astype(F32)
                up = up + gu_recv[i, 1, :, a:b].astype(F32)
            h_all[k, :, a:b] = (silu(scale * gate) * (scale * up)).astype(BF16)
            mine = h_all.at[k, :, pl.ds(a, b - a)]
            hiddens.append(reserve(3))
            for t in (near,) if c in RELAYED_HIDDEN else (far, near):
                remote(mine, mine, {"kv": t}, hiddens[c] + slot)
            remote(mine, mine, {"kv": partner}, hiddens[c])
        down_load.wait()
        acc = None
        for c, (a, b) in enumerate(fspans):
            blocks = [h_all.at[i, :, pl.ds(a, b - a)] for i in (partner, near, far)]
            for i in (1, 2):
                arrived(blocks[i], hiddens[c] + i)
            if c in RELAYED_HIDDEN:
                copies = [
                    described(
                        blocks[i], blocks[i], {"kv": partner}, hiddens[c] + i, inner_pending
                    )
                    for i in (1, 2)
                ]

                @pl.when(inner)
                def _():
                    for copy in copies:
                        copy.start()

            arrived(blocks[0], hiddens[c])
            product = jnp.dot(
                h_all[:, :, a:b].reshape(B, b - a),
                ref[p + "d_v"][a:b, :],
                preferred_element_type=F32,
            )
            acc = product if acc is None else acc + product
        return acc

    mixer = mixer_paired if paired else mixer_direct

    def scatter_rows(p, value):
        send, recv = ref[p + "_send"], ref[p + "_recv"]
        send[...] = value.astype(BF16).reshape(R, mr, d)
        copies = []
        for o in range(1, R):
            t, device = row_peer(o)
            copies.append(remote(send.at[t], recv.at[o - 1], device))
        wait_all(copies)
        total = send[r].astype(F32)
        for o in range(1, R):
            total = total + recv[o - 1].astype(F32)
        return total

    def reduce_rows_twice(p, value, buf, factor, out):
        total = scatter_rows(p, value)
        out[r] = (buf[r].astype(F32) + factor * total).astype(BF16)
        wait_all(gather_rows(out.at[r], out))

    def reduce_rows_once(p, value, buf, factor, out):
        whole, send, recv, parts = ref["rows_f"], ref[p + "_send"], ref[p + "_recv"], ref[p + "_parts"]
        whole[...] = value.reshape(DP, TP, mr, d)
        firsts, seconds = [], []
        spans_d = spans(d, 2)
        for a, b in spans_d:
            send[:, :, a:b] = whole[:, 1 - tp_i, :, a:b].astype(BF16)
            cut = (slice(None), slice(None), pl.ds(a, b - a))
            firsts.append(remote(send.at[cut], recv.at[cut], {"tp": 1 - tp_i}))
        for (a, b), first in zip(spans_d, firsts):
            first.wait_recv()
            chip = whole[:, tp_i, :, a:b] + recv[:, :, a:b].astype(F32)
            parts[dp_i, tp_i, :, :, a:b] = chip.astype(BF16)
            mine = parts.at[dp_i, tp_i, :, :, pl.ds(a, b - a)]
            for o in sorted(range(1, R), key=lambda o: o % TP == 0):
                seconds.append(remote(mine, mine, row_peer(o)[1]))
        wait_all(seconds)
        for j in range(DP):
            for c in range(TP):
                total = parts[0, c, j].astype(F32)
                for x in range(1, DP):
                    total = total + parts[x, c, j].astype(F32)
                i = j * TP + c
                out[i] = (buf[i].astype(F32) + factor * total).astype(BF16)

    reduce_rows = reduce_rows_once if DP == 2 and TP == 2 else reduce_rows_twice

    x_copies = gather_rows(ref["x"], ref["x_all"])
    own_x.wait()
    load_g1.wait()
    wait_all(x_copies)
    reduce_rows("p1", mixer("l", ref["x_all"], ref["g1_v"], lead), ref["x_all"], 0.5, ref["a_all"])
    for copy in load_attn:
        copy.wait()

    squares = normalised(ref["a_all"], ref["g2_v"])
    f_send, f_recv = ref["f_send"], ref["f_recv"]
    q_send, q_recv = ref["q_send"], ref["q_recv"]
    v_send, v_recv = ref["v_send"], ref["v_recv"]

    def project(name):
        return jnp.dot(ref["scaled"][...], ref[name + "_v"][...], preferred_element_type=F32)

    f_send[:, :, Wp:] = squares
    f_send[:, :, :W] = project("wf").reshape(K, mk, W)
    f_copies, q_copies, v_copies = [], [], []
    for o in kv_order:
        t, device = kv_peer(o)
        f_copies.append(remote(f_send.at[t], f_recv.at[o - 1], device))
    q_send[:, 0, :, :W] = project("wq").astype(BF16).reshape(K, mk, W)
    q_send[:, 1, :, :W] = project("wk").astype(BF16).reshape(K, mk, W)
    for o in kv_order:
        t, device = kv_peer(o)
        q_copies.append(remote(q_send.at[t], q_recv.at[o - 1], device))
    v_send[:, 0] = project("wv").astype(BF16).reshape(K, mk, V)
    v_send[:, 1] = project("wg").astype(BF16).reshape(K, mk, V)
    for o in kv_order:
        t, device = kv_peer(o)
        v_copies.append(remote(v_send.at[t], v_recv.at[o - 1], device))
    for copy in load_state:
        copy.wait()
    wait_all(f_copies)
    forget = f_send[k]
    for o in kv_order:
        forget = forget + f_recv[o - 1]
    scale = row_scale(forget[:, Wp:])
    forget = scale * forget[:, :W]
    decay = jnp.exp(
        (jnp.minimum(forget, 0.0) - jnp.log1p(jnp.exp(-jnp.abs(forget)))) / 16.0 + ref["eld_v"][...]
    )
    columns = ref["columns"]
    columns[0] = decay.T
    wait_all(q_copies)
    pair = []
    for i in range(2):
        total = q_send[k, i, :, :W].astype(F32)
        for o in kv_order:
            total = total + q_recv[o - 1, i, :, :W].astype(F32)
        pair.append(scale * total)
    columns[1] = pair[1].T
    columns[2] = (pair[0] * KEY_CHANNELS ** (-0.5)).T
    wait_all(v_copies)
    pair = []
    for i in range(2):
        total = v_send[k, i].astype(F32)
        for o in kv_order:
            total = total + v_recv[o - 1, i].astype(F32)
        pair.append(scale * total)
    ref["vals"][...] = pair[0]
    gates = silu(pair[1])
    for b in range(mk):
        for h in range(heads):
            rows = slice(h * KEY_CHANNELS, (h + 1) * KEY_CHANNELS)
            lanes = slice(h * VALUE_DIM, (h + 1) * VALUE_DIM)
            new = (
                columns[0, rows, b : b + 1] * ref["st_v"][b, h]
                + columns[1, rows, b : b + 1] * ref["vals"][b : b + 1, lanes]
            )
            ref["new_state"][b, h] = new
            ref["read"][b : b + 1, lanes] = jnp.sum(
                columns[2, rows, b : b + 1] * new, axis=0, keepdims=True
            )
    hr_all = ref["hr_all"]
    for h in range(heads):
        lanes = slice(h * VALUE_DIM, (h + 1) * VALUE_DIM)
        out = ref["read"][:, lanes]
        out = out * lax.rsqrt(jnp.mean(out * out, axis=1, keepdims=True) + epsilon)
        hr_all[k, :, lanes] = (out * ref["hng_v"][...] * gates[:, lanes]).astype(BF16)
    hr_copies = [remote(hr_all.at[k], hr_all.at[k], kv_peer(o)[1]) for o in kv_order]
    load_out.wait()
    wait_all(hr_copies)
    mixed = jnp.dot(hr_all[...].reshape(B, V), ref["wo_v"][...], preferred_element_type=F32)
    reduce_rows("p2", mixed, ref["a_all"], 1.0, ref["s_all"])
    load_g3.wait()

    share = scatter_rows("p3", mixer("t", ref["s_all"], ref["g3_v"], trail))
    ref["result"][...] = (ref["s_all"][r].astype(F32) + 0.5 * share).astype(BF16)
    for copy in pending:
        copy.wait_send()
    if paired:

        @pl.when(inner)
        def _():
            for copy in inner_pending:
                copy.wait_send()

        @pl.when(outer)
        def _():
            for copy in outer_pending:
                copy.wait_send()


ARGS = ("x", "st", "eld", "g1", "lg", "lu", "ld", "g2", "wq", "wk")
ARGS += ("wv", "wg", "wf", "hng", "wo", "g3", "tg", "tu", "td")


def per_device(sizes, *arrays):
    dp, tp, K = sizes
    R = dp * tp
    ref = dict(zip(ARGS, arrays))
    for n in ("g1", "g2", "g3", "hng"):
        ref[n] = ref[n].reshape(1, -1)
    mr, d = ref["x"].shape
    B, D = mr * R, d * K
    mk = B // K
    F = ref["lg"].shape[1]
    W, V = ref["wq"].shape[1], ref["wv"].shape[1]
    heads = W // KEY_CHANNELS
    Wp = padded(W)
    dims = (R, K, tp, D, B, d, F, W, V, heads)
    vm = {}
    for n in ARGS:
        if n != "x":
            vm[n + "_v"] = (ref[n].shape, ref[n].dtype)
    for n in ("x_all", "a_all", "s_all"):
        vm[n] = ((R, mr, d), BF16)
    vm["scaled"] = ((B, d), BF16)
    for p in ("l", "t"):
        vm[p + "gu_send"] = ((K, 2, mk, F), BF16)
        vm[p + "gu_recv"] = ((K - 1, 2, mk, F), BF16)
        vm[p + "ss_send"] = ((K, mk, LANES), F32)
        vm[p + "ss_recv"] = ((K - 1, mk, LANES), F32)
        vm[p + "h_all"] = ((K, mk, F), BF16)
        if K == PAIRS:
            vm[p + "relay"] = ((2, 2, mk, F), BF16)
    if K == PAIRS:
        vm["gu_f"] = ((K, 2, mk, F), F32)
    once = dp == 2 and tp == 2
    if once:
        vm["rows_f"] = ((dp, tp, mr, d), F32)
    for p in ("p1", "p2", "p3"):
        if once and p != "p3":
            vm[p + "_send"] = ((dp, mr, d), BF16)
            vm[p + "_recv"] = ((dp, mr, d), BF16)
            vm[p + "_parts"] = ((dp, tp, dp, mr, d), BF16)
        else:
            vm[p + "_send"] = ((R, mr, d), BF16)
            vm[p + "_recv"] = ((R - 1, mr, d), BF16)
    vm["f_send"] = ((K, mk, Wp + LANES), F32)
    vm["f_recv"] = ((K - 1, mk, Wp + LANES), F32)
    vm["q_send"] = ((K, 2, mk, Wp), BF16)
    vm["q_recv"] = ((K - 1, 2, mk, Wp), BF16)
    vm["v_send"] = ((K, 2, mk, V), BF16)
    vm["v_recv"] = ((K - 1, 2, mk, V), BF16)
    vm["columns"] = ((3, W, mk), F32)
    vm["vals"] = ((mk, V), F32)
    vm["read"] = ((mk, V), F32)
    vm["hr_all"] = ((K, mk, V), BF16)
    names = [*ARGS, "result", "new_state", *vm, "local_sem", "send_sem", "recv_sem"]
    sems = 4 * 2 * R + 2 * K * (1 + 3 * CHUNKS) + 4 * K
    return pl.pallas_call(
        functools.partial(kernel, dims, names),
        out_shape=(
            pltpu.VMEM((mr, d), BF16),
            pltpu.VMEM(ref["st"].shape, F32),
        ),
        in_specs=[pl.BlockSpec(memory_space=pl.ANY)] * len(ARGS),
        out_specs=[pl.BlockSpec(memory_space=pltpu.VMEM)] * 2,
        scratch_shapes=[
            *[pltpu.VMEM(shape, dtype) for shape, dtype in vm.values()],
            pltpu.SemaphoreType.DMA((20 + 6 * CHUNKS,)),
            pltpu.SemaphoreType.DMA((sems,)),
            pltpu.SemaphoreType.DMA((sems,)),
        ],
        compiler_params=pltpu.CompilerParams(
            collective_id=0, has_side_effects=True, vmem_limit_bytes=56 * 1024 * 1024
        ),
    )(*[ref[n] for n in ARGS])


def solution(mesh):
    sizes = (mesh.shape["dp"], mesh.shape["tp"], mesh.shape["kv"])
    return jax.shard_map(
        functools.partial(per_device, sizes),
        mesh=mesh,
        in_specs=(
            P(("grp", "dp", "tp"), "kv"),
            P(("grp", "kv"), ("dp", "tp"), None, None),
            P(("grp", "kv"), ("dp", "tp")),
            P("kv"),
            P("kv", ("dp", "tp")),
            P("kv", ("dp", "tp")),
            P(("dp", "tp"), "kv"),
            P("kv"),
            P("kv", ("dp", "tp")),
            P("kv", ("dp", "tp")),
            P("kv", ("dp", "tp")),
            P("kv", ("dp", "tp")),
            P("kv", ("dp", "tp")),
            P(),
            P(("dp", "tp"), "kv"),
            P("kv"),
            P("kv", ("dp", "tp")),
            P("kv", ("dp", "tp")),
            P(("dp", "tp"), "kv"),
        ),
        out_specs=(P(("grp", "dp", "tp"), "kv"), P(("grp", "kv"), ("dp", "tp"), None, None)),
        check_vma=False,
    )
```

```python
import functools

import jax
import jax.numpy as jnp
from jax import lax
from jax.experimental import pallas as pl
from jax.experimental.pallas import tpu as pltpu
from jax.sharding import PartitionSpec as P

KEY_CHANNELS = 64
VALUE_DIM = 128
LANES = 128
epsilon = 1e-06
MESH = pl.DeviceIdType.MESH
F32 = jnp.float32
BF16 = jnp.bfloat16
CHUNKS = 4
PAIRS = 4
SHARES = (3, 4, 4)
RELAYED_SUMS = (3, 3)
RELAYED_HIDDEN = ((0, 1), ())
FIRST = (8.9, 9.8, 10.9, 13.0, 14.0, 16.0, 17.0, 19.0, 22.0, 23.0, 25.0, 28.0, 30.0, 32.0)
FIRST += (33.0, 33.1, 35.0, 38.0, 39.0, 40.0, 41.0, 43.0, 44.0, 44.1, 49.0, 50.0, 52.0, 54.0)
FIRST += (54.1, 54.2, 55.0, 57.0, 59.0, 62.0, 64.0, 67.0, 69.0, 71.0, 74.0)
SECOND = (15.0, 18.0, 20.0, 21.0, 24.0, 26.0, 27.0, 33.2, 33.3, 36.0, 36.1, 36.2, 37.0, 37.1)
SECOND += (42.0, 45.0, 46.0, 47.0, 48.0, 51.0, 53.0, 53.1, 56.0, 58.0, 60.0, 61.0, 63.0, 65.0)
SECOND += (66.0, 71.1, 71.2, 73.0, 73.1, 73.2, 75.0)
READY = (FIRST, SECOND)


def spans(width, count):
    if width % LANES:
        return [(0, width)]
    tile = 2 * LANES if width % (2 * LANES) == 0 else LANES
    tiles = width // tile
    count = min(count, tiles)
    cuts = [tile * ((tiles * i + count - 1) // count) for i in range(count + 1)]
    return list(zip(cuts[:-1], cuts[1:]))


def shared(width, shares):
    tile = 2 * LANES
    tiles = width // tile
    if width % tile or tiles < sum(shares):
        return spans(width, len(shares))
    ends = [sum(shares[: i + 1]) for i in range(len(shares))]
    cuts = [0] + [tile * (tiles * end // sum(shares)) for end in ends]
    return list(zip(cuts[:-1], cuts[1:]))


def padded(width):
    return -(-width // LANES) * LANES


def silu(x):
    return x * jax.nn.sigmoid(x)


def kernel(dims, names, *refs):
    R, K, TP, D, B, d, F, W, V, heads, S = dims
    DP = R // TP
    rows, hr, hm = B // S, B // R // S, B // K // S
    ref = dict(zip(names, refs))
    dp_i, tp_i, k = lax.axis_index("dp"), lax.axis_index("tp"), lax.axis_index("kv")
    r = dp_i * TP + tp_i
    Wp = padded(W)
    kv_order = sorted(range(1, K), key=lambda o: abs(2 * o - K))
    counter = {"send": 0, "recv": 0, "local": 0}
    pending, inner_pending, outer_pending = [], [], []
    waited = set()
    paired = K == PAIRS
    if paired:
        side = k // 2
        partner = k + 1 - 2 * lax.rem(k, 2)
        near, far = 2 - side, 3 * (1 - side)
        across = 2 * (1 - side)
        inner = lax.rem(k + 1, K) // 2 == 1
        outer = jnp.logical_not(inner)
        slot = jnp.where(inner, 1, 2)

    def row_peer(o):
        t = lax.rem(r + o, R)
        return t, {"dp": t // TP, "tp": lax.rem(t, TP)}

    def kv_peer(o):
        t = lax.rem(k + o, K)
        return t, {"kv": t}

    def local(src, dst):
        i = counter["local"]
        counter["local"] += 1
        copy = pltpu.make_async_copy(src, dst, ref["local_sem"].at[i])
        copy.start()
        return copy

    def loaded(*copies):
        for copy in copies:
            if id(copy) not in waited:
                waited.add(id(copy))
                copy.wait()

    def group():
        pair = counter["send"], counter["recv"]
        counter["send"] += 1
        counter["recv"] += 1
        return pair

    def arrival():
        counter["recv"] += 1
        return counter["recv"] - 1

    def described(src, dst, device, sems):
        return pltpu.make_async_remote_copy(
            src_ref=src,
            dst_ref=dst,
            send_sem=ref["send_sem"].at[sems[0]],
            recv_sem=ref["recv_sem"].at[sems[1]],
            device_id=device,
            device_id_type=MESH,
        )

    def remote(src, dst, device, sems):
        described(src, dst, device, sems).start()

    def arrived(block, sems):
        described(block, block, row_peer(1)[1], (0, sems[1])).wait_recv()

    def left(block, sems):
        described(block, block, row_peer(1)[1], (sems[0], 0)).wait_send()

    def to_kv_peers(block_of, recv, like):
        sems = group()
        for o in kv_order:
            t, device = kv_peer(o)
            remote(block_of(t), recv(o), device, sems)
        pending.append((like, sems))
        return sems

    own_x = [local(ref["x"].at[pl.ds(s * hr, hr)], ref["x_all", s].at[r]) for s in range(S)]
    load_g1 = local(ref["g1"], ref["g1_v"])
    fspans = shared(F, SHARES) if paired else spans(F, CHUNKS)

    def load_mixer(p):
        first = []
        for a, b in fspans:
            cut = (slice(None), slice(None)) if b - a == F else (slice(None), pl.ds(a, b - a))
            first.append(
                (
                    local(ref[p + "g"].at[cut], ref[p + "g_v"].at[cut]),
                    local(ref[p + "u"].at[cut], ref[p + "u_v"].at[cut]),
                )
            )
        return first, local(ref[p + "d"], ref[p + "d_v"])

    lead = load_mixer("l")
    load_attn = [local(ref[n], ref[n + "_v"]) for n in ("g2", "wq", "wk", "wf", "wv", "wg")]
    load_state = [local(ref[n], ref[n + "_v"]) for n in ("st", "eld", "hng")]
    load_out = local(ref["wo"], ref["wo_v"])
    load_g3 = local(ref["g3"], ref["g3_v"])
    trail = load_mixer("t")

    barrier = pltpu.get_barrier_semaphore()
    for o in range(1, R):
        pl.semaphore_signal(barrier, inc=1, device_id=row_peer(o)[1], device_id_type=MESH)
    for o in kv_order:
        pl.semaphore_signal(barrier, inc=1, device_id=kv_peer(o)[1], device_id_type=MESH)
    pl.semaphore_wait(barrier, R - 1 + K - 1)

    def gather_rows(buf):
        sems = group()
        for o in range(1, R):
            remote(buf.at[r], buf.at[r], row_peer(o)[1], sems)
        pending.append((buf.at[pl.ds(0, R - 1)], sems))
        return sems

    def flat(block):
        if hm % 16 == 0:
            return block.reshape(rows, -1)
        return block.astype(F32).reshape(rows, -1).astype(BF16)

    def normalised(s, buf, gain):
        wide = buf[...].astype(F32).reshape(rows, d)
        squares = jnp.sum(wide * wide, axis=1, keepdims=True)
        ref["scaled", s][...] = (wide * gain[...]).astype(BF16)
        return jnp.broadcast_to(squares, (rows, LANES)).reshape(K, hm, LANES)

    def row_scale(total):
        return lax.rsqrt(total / D + epsilon)[:, :1]

    def part(buf, i, a, b):
        return buf.at[i] if b - a == F else buf.at[i, :, :, pl.ds(a, b - a)]

    def piece(buf, i, a, b):
        return buf.at[i] if b - a == F else buf.at[i, :, pl.ds(a, b - a)]

    def send_squares(p, s, buf, gain):
        ss_send, ss_recv = ref[p, "ss_send", s], ref[p, "ss_recv", s]
        ss_send[...] = normalised(s, buf, gain)
        return to_kv_peers(
            lambda t: ss_send.at[t], lambda o: ss_recv.at[o - 1], ss_send.at[pl.ds(0, K - 1)]
        )

    def total_scale(p, s, sems):
        arrived(ref[p, "ss_recv", s], sems)
        total = ref[p, "ss_send", s][k]
        for o in kv_order:
            total = total + ref[p, "ss_recv", s][o - 1]
        return row_scale(total)

    def mixer_direct(p, s, buf, gain, loads):
        gu_loads, down_load = loads
        gu_send, gu_recv, h_all = ref[p, "gu_send", s], ref[p, "gu_recv", s], ref[p, "h_all", s]
        loaded(load_g1, load_g3)
        ss_sems = send_squares(p, s, buf, gain)
        gu_sems = []
        for (a, b), pair in zip(fspans, gu_loads):
            for i, name in enumerate("gu"):
                loaded(pair[i])
                product = jnp.dot(
                    ref["scaled", s][...], ref[p + name + "_v"][:, a:b], preferred_element_type=F32
                )
                gu_send[:, i, :, a:b] = product.reshape(K, hm, b - a).astype(BF16)
            gu_sems.append(
                to_kv_peers(
                    lambda t: part(gu_send, t, a, b),
                    lambda o: part(gu_recv, o - 1, a, b),
                    part(gu_send, pl.ds(0, K - 1), a, b),
                )
            )
        scale = total_scale(p, s, ss_sems)
        h_sems = []
        for (a, b), sems in zip(fspans, gu_sems):
            arrived(part(gu_recv, pl.ds(0, K - 1), a, b), sems)
            gate = gu_send[k, 0, :, a:b].astype(F32)
            up = gu_send[k, 1, :, a:b].astype(F32)
            for o in kv_order:
                gate = gate + gu_recv[o - 1, 0, :, a:b].astype(F32)
                up = up + gu_recv[o - 1, 1, :, a:b].astype(F32)
            h_all[k, :, a:b] = (silu(scale * gate) * (scale * up)).astype(BF16)
            mine = piece(h_all, k, a, b)
            h_sems.append(
                to_kv_peers(lambda t: mine, lambda o: mine, piece(h_all, pl.ds(0, K - 1), a, b))
            )
        loaded(down_load)
        acc = None
        for (a, b), sems in zip(fspans, h_sems):
            arrived(piece(h_all, pl.ds(0, K - 1), a, b), sems)
            product = jnp.dot(
                flat(h_all[:, :, a:b]), ref[p + "d_v"][a:b, :], preferred_element_type=F32
            )
            acc = product if acc is None else acc + product
        return acc
        yield

    def mixer_paired(p, s, buf, gain, loads):
        gu_loads, down_load = loads
        gu_f, gu_send, gu_recv = ref["gu_f", s], ref[p, "gu_send", s], ref[p, "gu_recv", s]
        relay, h_all = ref[p, "relay", s], ref[p, "h_all", s]
        loaded(load_g1 if p == "l" else load_g3)
        ss_sems = send_squares(p, s, buf, gain)
        sums, relays, hiddens = [], [], [None] * len(fspans)
        relayed, forwarded = RELAYED_SUMS[s], RELAYED_HIDDEN[s]

        def to_partner(c):
            a, b = fspans[c]
            remote(part(gu_send, partner, a, b), part(gu_recv, 0, a, b), {"kv": partner}, sums[c])
            pending.append((part(gu_send, pl.ds(0, 3), a, b), sums[c]))

        for c, ((a, b), pair) in enumerate(zip(fspans, gu_loads)):
            if c:
                yield
            for i, name in enumerate("gu"):
                loaded(pair[i])
                product = jnp.dot(
                    ref["scaled", s][...], ref[p + name + "_v"][:, a:b], preferred_element_type=F32
                ).reshape(K, hm, b - a)
                gu_f[:, i, :, a:b] = product
                gu_send[:, i, :, a:b] = product.astype(BF16)
            sums.append(group())
            if c < relayed:
                relays.append(arrival())
                cut = (pl.ds(across, 2), slice(None), slice(None), pl.ds(a, b - a))
                where = (slice(None), slice(None), slice(None), pl.ds(a, b - a))
                copy = described(
                    gu_send.at[cut], relay.at[where], {"kv": partner}, (sums[c][0], relays[c])
                )
                pl.when(outer)(copy.start)
            else:
                for t in (far, near):
                    remote(
                        part(gu_send, t, a, b), part(gu_recv, slot, a, b), {"kv": t}, sums[c]
                    )
            if c:
                to_partner(c - 1)
        to_partner(len(fspans) - 1)

        def pass_on(c):
            a, b = fspans[c]
            where = (slice(None), slice(None), slice(None), pl.ds(a, b - a))
            onward = [
                described(part(gu_send, t, a, b), part(gu_recv, 1, a, b), {"kv": t}, sums[c])
                for t in (far, near)
            ]

            @pl.when(inner)
            def _():
                arrived(relay.at[where], (0, relays[c]))
                both = gu_f[pl.ds(across, 2), :, :, a:b] + relay[:, :, :, a:b].astype(F32)
                gu_send[pl.ds(across, 2), :, :, a:b] = both.astype(BF16)
                for copy in onward:
                    copy.start()

        for c in range(relayed):
            yield
            pass_on(c)
        yield
        scale = total_scale(p, s, ss_sems)
        for c, (a, b) in enumerate(fspans):
            if c:
                yield
            gate, up = gu_f[k, 0, :, a:b], gu_f[k, 1, :, a:b]
            blocks = 2 if c < relayed else 3
            arrived(part(gu_recv, pl.ds(0, blocks), a, b), sums[c])
            for i in range(blocks):
                gate = gate + gu_recv[i, 0, :, a:b].astype(F32)
                up = up + gu_recv[i, 1, :, a:b].astype(F32)
            h_all[k, :, a:b] = (silu(scale * gate) * (scale * up)).astype(BF16)
            mine = h_all.at[k, :, pl.ds(a, b - a)]
            hiddens[c] = group()
            for t in (near, partner) if c in forwarded else (far, near, partner):
                remote(mine, mine, {"kv": t}, hiddens[c])
            if c in forwarded:
                inner_pending.append((h_all.at[:, :, pl.ds(a, b - a)], hiddens[c]))
                outer_pending.append((h_all.at[pl.ds(0, 2), :, pl.ds(a, b - a)], hiddens[c]))
            else:
                pending.append((h_all.at[pl.ds(0, 3), :, pl.ds(a, b - a)], hiddens[c]))
        for c in forwarded:
            yield
            a, b = fspans[c]
            blocks = [h_all.at[i, :, pl.ds(a, b - a)] for i in (near, far)]
            copies = [described(block, block, {"kv": partner}, hiddens[c]) for block in blocks]

            @pl.when(inner)
            def _():
                arrived(h_all.at[pl.ds(0, 3), :, pl.ds(a, b - a)], hiddens[c])
                for copy in copies:
                    copy.start()

        acc = None
        for c, (a, b) in enumerate(fspans):
            yield
            loaded(down_load)
            if c in forwarded:

                @pl.when(outer)
                def _():
                    arrived(h_all.at[pl.ds(0, 3), :, pl.ds(a, b - a)], hiddens[c])

            else:
                arrived(h_all.at[pl.ds(0, 3), :, pl.ds(a, b - a)], hiddens[c])
            product = jnp.dot(
                flat(h_all[:, :, a:b]), ref[p + "d_v"][a:b, :], preferred_element_type=F32
            )
            acc = product if acc is None else acc + product
        return acc

    mixer = mixer_paired if paired else mixer_direct

    def scatter_rows(p, s, value):
        send, recv = ref[p, "_send", s], ref[p, "_recv", s]
        send[...] = value.reshape(R, hr, d).astype(BF16)
        sems = group()
        for o in range(1, R):
            t, device = row_peer(o)
            remote(send.at[t], recv.at[o - 1], device, sems)
        pending.append((send.at[pl.ds(0, R - 1)], sems))
        return sems

    def scattered(p, s, sems):
        send, recv = ref[p, "_send", s], ref[p, "_recv", s]
        arrived(recv, sems)
        total = send[r].astype(F32)
        for o in range(1, R):
            total = total + recv[o - 1].astype(F32)
        return total

    def reduce_rows_twice(p, s, value, buf, factor, out):
        total = scattered(p, s, scatter_rows(p, s, value))
        out[r] = (buf[r].astype(F32) + factor * total).astype(BF16)
        arrived(out.at[pl.ds(0, R - 1)], gather_rows(out))
        return
        yield

    def reduce_rows_once(p, s, value, buf, factor, out):
        whole, send, recv, parts = ref["rows_f", s], ref[p, "_send", s], ref[p, "_recv", s], ref[p, "_parts", s]
        whole[...] = value.reshape(DP, TP, hr, d)
        first, second = group(), group()
        halves = [first[1], arrival()]
        spans_d = spans(d, 2)
        for a, b in spans_d:
            send[:, :, a:b] = whole[:, 1 - tp_i, :, a:b].astype(BF16)
            cut = (slice(None), slice(None), pl.ds(a, b - a))
            remote(send.at[cut], recv.at[cut], {"tp": 1 - tp_i}, (first[0], halves[a > 0]))
        pending.append((send, first))
        for (a, b), half in zip(spans_d, halves):
            yield
            arrived(recv.at[:, :, pl.ds(a, b - a)], (0, half))
            chip = whole[:, tp_i, :, a:b] + recv[:, :, a:b].astype(F32)
            parts[r, :, :, a:b] = chip.astype(BF16)
            mine = parts.at[r, :, :, pl.ds(a, b - a)]
            for o in sorted(range(1, R), key=lambda o: o % TP == 0):
                remote(mine, mine, row_peer(o)[1], second)
        pending.append((parts.at[pl.ds(0, R - 1)], second))
        yield
        arrived(parts.at[pl.ds(0, R - 1)], second)
        for j in range(DP):
            for c in range(TP):
                total = parts[c, j].astype(F32)
                for x in range(1, DP):
                    total = total + parts[x * TP + c, j].astype(F32)
                i = j * TP + c
                out[i] = (buf[i].astype(F32) + factor * total).astype(BF16)

    reduce_rows = reduce_rows_once if DP == 2 and TP == 2 else reduce_rows_twice

    def chain(s):
        x_all, a_all, s_all = ref["x_all", s], ref["a_all", s], ref["s_all", s]
        loaded(own_x[s])
        sems = gather_rows(x_all)
        yield
        arrived(x_all.at[pl.ds(0, R - 1)], sems)
        mixed = yield from mixer("l", s, x_all, ref["g1_v"], lead)
        yield from reduce_rows("p1", s, mixed, x_all, 0.5, a_all)

        loaded(*load_attn)
        squares = normalised(s, a_all, ref["g2_v"])
        f_send, f_recv = ref["f_send", s], ref["f_recv", s]
        q_send, q_recv = ref["q_send", s], ref["q_recv", s]
        v_send, v_recv = ref["v_send", s], ref["v_recv", s]

        def project(name, width):
            return jnp.dot(
                ref["scaled", s][...], ref[name + "_v"][...], preferred_element_type=F32
            ).reshape(K, hm, width)

        f_send[:, :, Wp:] = squares
        f_send[:, :, :W] = project("wf", W)

        def exchange(send, recv):
            return to_kv_peers(
                lambda t: send.at[t], lambda o: recv.at[o - 1], send.at[pl.ds(0, K - 1)]
            )

        f_sems = exchange(f_send, f_recv)
        q_send[:, 0, :, :W] = project("wq", W).astype(BF16)
        q_send[:, 1, :, :W] = project("wk", W).astype(BF16)
        q_sems = exchange(q_send, q_recv)
        v_send[:, 0] = project("wv", V).astype(BF16)
        v_send[:, 1] = project("wg", V).astype(BF16)
        v_sems = exchange(v_send, v_recv)
        yield
        loaded(*load_state)
        arrived(f_recv, f_sems)
        forget = f_send[k]
        for o in kv_order:
            forget = forget + f_recv[o - 1]
        scale = row_scale(forget[:, Wp:])
        forget = scale * forget[:, :W]
        mine = slice(s * hm, (s + 1) * hm)
        decay = jnp.exp(
            (jnp.minimum(forget, 0.0) - jnp.log1p(jnp.exp(-jnp.abs(forget)))) / 16.0
            + ref["eld_v"][mine]
        )
        columns, read, vals = ref["columns", s], ref["read", s], ref["vals", s]
        columns[0] = decay.T
        yield
        arrived(q_recv, q_sems)
        pair = []
        for i in range(2):
            total = q_send[k, i, :, :W].astype(F32)
            for o in kv_order:
                total = total + q_recv[o - 1, i, :, :W].astype(F32)
            pair.append(scale * total)
        queries = pair[0] * KEY_CHANNELS ** (-0.5)
        columns[1] = pair[1].T
        columns[2] = (queries * decay).T
        overlap = queries * pair[1]
        for b in range(hm):
            for h in range(heads):
                keys = slice(h * KEY_CHANNELS, (h + 1) * KEY_CHANNELS)
                lanes = slice(h * VALUE_DIM, (h + 1) * VALUE_DIM)
                read[b : b + 1, lanes] = jnp.sum(
                    columns[2, keys, b : b + 1] * ref["st_v"][s * hm + b, h], axis=0, keepdims=True
                )
        yield
        arrived(v_recv, v_sems)
        pair = []
        for i in range(2):
            total = v_send[k, i].astype(F32)
            for o in kv_order:
                total = total + v_recv[o - 1, i].astype(F32)
            pair.append(scale * total)
        vals[...] = pair[0]
        gates = silu(pair[1])
        hr_all = ref["hr_all", s]
        for h in range(heads):
            lanes = slice(h * VALUE_DIM, (h + 1) * VALUE_DIM)
            keys = slice(h * KEY_CHANNELS, (h + 1) * KEY_CHANNELS)
            out = read[:, lanes] + (
                jnp.sum(overlap[:, keys], axis=1, keepdims=True) * pair[0][:, lanes]
            )
            out = out * lax.rsqrt(jnp.mean(out * out, axis=1, keepdims=True) + epsilon)
            hr_all[k, :, lanes] = (out * ref["hng_v"][...] * gates[:, lanes]).astype(BF16)
        hr_sems = to_kv_peers(
            lambda t: hr_all.at[k], lambda o: hr_all.at[k], hr_all.at[pl.ds(0, K - 1)]
        )
        yield
        for b in range(hm):
            for h in range(heads):
                keys = slice(h * KEY_CHANNELS, (h + 1) * KEY_CHANNELS)
                lanes = slice(h * VALUE_DIM, (h + 1) * VALUE_DIM)
                ref["new_state"][s * hm + b, h] = (
                    columns[0, keys, b : b + 1] * ref["st_v"][s * hm + b, h]
                    + columns[1, keys, b : b + 1] * vals[b : b + 1, lanes]
                )
        yield
        loaded(load_out)
        arrived(hr_all.at[pl.ds(0, K - 1)], hr_sems)
        mixed = jnp.dot(flat(hr_all[...]), ref["wo_v"][...], preferred_element_type=F32)
        yield from reduce_rows("p2", s, mixed, a_all, 1.0, s_all)

        mixed = yield from mixer("t", s, s_all, ref["g3_v"], trail)
        sems = scatter_rows("p3", s, mixed)
        yield
        share = scattered("p3", s, sems)
        ref["result"][s * hr : (s + 1) * hr] = (s_all[r].astype(F32) + 0.5 * share).astype(BF16)

    chains = [chain(s) for s in range(S)]
    taken = {}
    for s, steps in enumerate(chains):
        next(steps)
        taken[s] = 0
    while taken:
        s = min(taken, key=lambda i: READY[i][taken[i]] if S > 1 else 0)
        if next(chains[s], chains) is chains:
            del taken[s]
        else:
            taken[s] += 1
    loaded(load_g3)
    for block, sems in pending:
        left(block, sems)
    if inner_pending:

        @pl.when(inner)
        def _():
            for block, sems in inner_pending:
                left(block, sems)

        @pl.when(outer)
        def _():
            for block, sems in outer_pending:
                left(block, sems)


ARGS = ("x", "st", "eld", "g1", "lg", "lu", "ld", "g2", "wq", "wk")
ARGS += ("wv", "wg", "wf", "hng", "wo", "g3", "tg", "tu", "td")


def store(result, state, result_out, state_out, sem):
    copies = [
        pltpu.make_async_copy(state, state_out, sem.at[0]),
        pltpu.make_async_copy(result, result_out, sem.at[1]),
    ]
    for copy in copies:
        copy.start()
    for copy in copies:
        copy.wait()


def per_device(sizes, *arrays):
    dp, tp, K = sizes
    R = dp * tp
    ref = dict(zip(ARGS, arrays))
    for n in ("g1", "g2", "g3", "hng"):
        ref[n] = ref[n].reshape(1, -1)
    mr, d = ref["x"].shape
    B, D = mr * R, d * K
    F = ref["lg"].shape[1]
    W, V = ref["wq"].shape[1], ref["wv"].shape[1]
    heads = W // KEY_CHANNELS
    Wp = padded(W)
    paired = K == PAIRS
    S = 2 if paired and mr * K == B and mr % 16 == 0 else 1
    rows, hr, hm = B // S, mr // S, B // K // S
    dims = (R, K, tp, D, B, d, F, W, V, heads, S)
    once = dp == 2 and tp == 2
    vm = {}
    for n in ARGS:
        if n != "x":
            vm[n + "_v"] = (ref[n].shape, ref[n].dtype)
    for s in range(S):
        for n in ("x_all", "a_all", "s_all"):
            vm[n, s] = ((R, hr, d), BF16)
        vm["scaled", s] = ((rows, d), BF16)
        for p in ("l", "t"):
            vm[p, "gu_send", s] = ((K, 2, hm, F), BF16)
            vm[p, "gu_recv", s] = ((K - 1, 2, hm, F), BF16)
            vm[p, "ss_send", s] = ((K, hm, LANES), F32)
            vm[p, "ss_recv", s] = ((K - 1, hm, LANES), F32)
            vm[p, "h_all", s] = ((K, hm, F), BF16)
            if paired:
                vm[p, "relay", s] = ((2, 2, hm, F), BF16)
        if paired:
            vm["gu_f", s] = ((K, 2, hm, F), F32)
        if once:
            vm["rows_f", s] = ((dp, tp, hr, d), F32)
        for p in ("p1", "p2", "p3"):
            if once and p != "p3":
                vm[p, "_send", s] = ((dp, hr, d), BF16)
                vm[p, "_recv", s] = ((dp, hr, d), BF16)
                vm[p, "_parts", s] = ((R, dp, hr, d), BF16)
            else:
                vm[p, "_send", s] = ((R, hr, d), BF16)
                vm[p, "_recv", s] = ((R - 1, hr, d), BF16)
        vm["f_send", s] = ((K, hm, Wp + LANES), F32)
        vm["f_recv", s] = ((K - 1, hm, Wp + LANES), F32)
        vm["q_send", s] = ((K, 2, hm, Wp), BF16)
        vm["q_recv", s] = ((K - 1, 2, hm, Wp), BF16)
        vm["v_send", s] = ((K, 2, hm, V), BF16)
        vm["v_recv", s] = ((K - 1, 2, hm, V), BF16)
        vm["columns", s] = ((3, W, hm), F32)
        vm["vals", s] = ((hm, V), F32)
        vm["read", s] = ((hm, V), F32)
        vm["hr_all", s] = ((K, hm, V), BF16)
    names = [*ARGS, "result", "new_state", *vm, "local_sem", "send_sem", "recv_sem"]
    chunks = len(SHARES) if paired else CHUNKS
    sems = S * (14 + 2 * (1 + 2 * chunks + max(RELAYED_SUMS)))
    outputs = pl.pallas_call(
        functools.partial(kernel, dims, names),
        out_shape=(
            pltpu.VMEM((mr, d), BF16),
            pltpu.VMEM(ref["st"].shape, F32),
        ),
        in_specs=[pl.BlockSpec(memory_space=pl.ANY)] * len(ARGS),
        out_specs=[pl.BlockSpec(memory_space=pltpu.VMEM)] * 2,
        scratch_shapes=[
            *[pltpu.VMEM(shape, dtype) for shape, dtype in vm.values()],
            pltpu.SemaphoreType.DMA((15 + S + 4 * chunks,)),
            pltpu.SemaphoreType.DMA((sems,)),
            pltpu.SemaphoreType.DMA((sems,)),
        ],
        compiler_params=pltpu.CompilerParams(
            collective_id=0, has_side_effects=True, vmem_limit_bytes=56 * 1024 * 1024
        ),
    )(*[ref[n] for n in ARGS])
    return pl.pallas_call(
        store,
        out_shape=(
            jax.ShapeDtypeStruct((mr, d), BF16),
            jax.ShapeDtypeStruct(ref["st"].shape, F32),
        ),
        in_specs=[pl.BlockSpec(memory_space=pltpu.VMEM)] * 2,
        out_specs=[pl.BlockSpec(memory_space=pl.ANY)] * 2,
        scratch_shapes=[pltpu.SemaphoreType.DMA((2,))],
    )(*[pltpu.with_memory_space_constraint(v, pltpu.VMEM) for v in outputs])


def solution(mesh):
    sizes = (mesh.shape["dp"], mesh.shape["tp"], mesh.shape["kv"])
    return jax.shard_map(
        functools.partial(per_device, sizes),
        mesh=mesh,
        in_specs=(
            P(("grp", "dp", "tp"), "kv"),
            P(("grp", "kv"), ("dp", "tp"), None, None),
            P(("grp", "kv"), ("dp", "tp")),
            P("kv"),
            P("kv", ("dp", "tp")),
            P("kv", ("dp", "tp")),
            P(("dp", "tp"), "kv"),
            P("kv"),
            P("kv", ("dp", "tp")),
            P("kv", ("dp", "tp")),
            P("kv", ("dp", "tp")),
            P("kv", ("dp", "tp")),
            P("kv", ("dp", "tp")),
            P(),
            P(("dp", "tp"), "kv"),
            P("kv"),
            P("kv", ("dp", "tp")),
            P("kv", ("dp", "tp")),
            P(("dp", "tp"), "kv"),
        ),
        out_specs=(P(("grp", "dp", "tp"), "kv"), P(("grp", "kv"), ("dp", "tp"), None, None)),
        check_vma=False,
    )
```

```python
import functools

import jax
import jax.numpy as jnp
from jax import lax
from jax.experimental import pallas as pl
from jax.experimental.pallas import tpu as pltpu
from jax.sharding import PartitionSpec as P

KEY_CHANNELS = 64
VALUE_DIM = 128
LANES = 128
epsilon = 1e-06
MESH = pl.DeviceIdType.MESH
F32 = jnp.float32
BF16 = jnp.bfloat16
CHUNKS = 4
PAIRS = 4
SHARES = (3, 4, 4)
RELAYED_SUMS = (3, 3)
RELAYED_HIDDEN = ((0, 1), ())
FIRST = (8.9, 9.8, 10.9, 13.0, 14.0, 16.0, 17.0, 19.0, 22.0, 23.0, 25.0, 28.0, 30.0, 32.0)
FIRST += (33.0, 35.0, 38.0, 39.0, 40.0, 41.0, 43.0, 44.0, 49.0, 50.0, 52.0, 54.0, 54.1, 54.2)
FIRST += (55.0, 57.0, 59.0, 62.0, 64.0, 67.0, 69.0, 71.0, 74.0)
SECOND = (15.0, 18.0, 20.0, 21.0, 24.0, 26.0, 27.0, 33.2, 33.3, 36.0, 36.1, 36.2, 37.0, 42.0)
SECOND += (45.0, 46.0, 47.0, 48.0, 51.0, 53.0, 56.0, 58.0, 60.0, 61.0, 63.0, 65.0, 66.0, 71.1)
SECOND += (71.2, 73.0, 73.1, 73.2, 75.0)
READY = (FIRST, SECOND)


def spans(width, count):
    if width % LANES:
        return [(0, width)]
    tile = 2 * LANES if width % (2 * LANES) == 0 else LANES
    tiles = width // tile
    count = min(count, tiles)
    cuts = [tile * ((tiles * i + count - 1) // count) for i in range(count + 1)]
    return list(zip(cuts[:-1], cuts[1:]))


def shared(width, shares):
    tile = 2 * LANES
    tiles = width // tile
    if width % tile or tiles < sum(shares):
        return spans(width, len(shares))
    ends = [sum(shares[: i + 1]) for i in range(len(shares))]
    cuts = [0] + [tile * (tiles * end // sum(shares)) for end in ends]
    return list(zip(cuts[:-1], cuts[1:]))


def padded(width):
    return -(-width // LANES) * LANES


def silu(x):
    return x * jax.nn.sigmoid(x)


def kernel(dims, names, *refs):
    R, K, TP, D, B, d, F, W, V, heads, S = dims
    DP = R // TP
    rows, hr, hm = B // S, B // R // S, B // K // S
    ref = dict(zip(names, refs))
    dp_i, tp_i, k = lax.axis_index("dp"), lax.axis_index("tp"), lax.axis_index("kv")
    r = dp_i * TP + tp_i
    Wp = padded(W)
    kv_order = sorted(range(1, K), key=lambda o: abs(2 * o - K))
    counter = {"send": 0, "recv": 0, "local": 0}
    pending, inner_pending, outer_pending = [], [], []
    waited = set()
    paired = K == PAIRS
    if paired:
        side = k // 2
        partner = k + 1 - 2 * lax.rem(k, 2)
        near, far = 2 - side, 3 * (1 - side)
        across = 2 * (1 - side)
        inner = lax.rem(k + 1, K) // 2 == 1
        outer = jnp.logical_not(inner)
        slot = jnp.where(inner, 1, 2)

    def row_peer(o):
        t = lax.rem(r + o, R)
        return t, {"dp": t // TP, "tp": lax.rem(t, TP)}

    def kv_peer(o):
        t = lax.rem(k + o, K)
        return t, {"kv": t}

    def local(src, dst):
        i = counter["local"]
        counter["local"] += 1
        copy = pltpu.make_async_copy(src, dst, ref["local_sem"].at[i])
        copy.start()
        return copy

    def loaded(*copies):
        for copy in copies:
            if id(copy) not in waited:
                waited.add(id(copy))
                copy.wait()

    def group():
        pair = counter["send"], counter["recv"]
        counter["send"] += 1
        counter["recv"] += 1
        return pair

    def arrival():
        counter["recv"] += 1
        return counter["recv"] - 1

    def described(src, dst, device, sems):
        return pltpu.make_async_remote_copy(
            src_ref=src,
            dst_ref=dst,
            send_sem=ref["send_sem"].at[sems[0]],
            recv_sem=ref["recv_sem"].at[sems[1]],
            device_id=device,
            device_id_type=MESH,
        )

    def remote(src, dst, device, sems):
        described(src, dst, device, sems).start()

    def arrived(block, sems):
        described(block, block, row_peer(1)[1], (0, sems[1])).wait_recv()

    def left(block, sems):
        described(block, block, row_peer(1)[1], (sems[0], 0)).wait_send()

    def to_kv_peers(block_of, recv, like):
        sems = group()
        for o in kv_order:
            t, device = kv_peer(o)
            remote(block_of(t), recv(o), device, sems)
        pending.append((like, sems))
        return sems

    own_x = [local(ref["x"].at[pl.ds(s * hr, hr)], ref["x_all", s].at[r]) for s in range(S)]
    load_g1 = local(ref["g1"], ref["g1_v"])
    fspans = shared(F, SHARES) if paired else spans(F, CHUNKS)

    def load_mixer(p):
        first = []
        for a, b in fspans:
            cut = (slice(None), slice(None)) if b - a == F else (slice(None), pl.ds(a, b - a))
            first.append(
                (
                    local(ref[p + "g"].at[cut], ref[p + "g_v"].at[cut]),
                    local(ref[p + "u"].at[cut], ref[p + "u_v"].at[cut]),
                )
            )
        return first, local(ref[p + "d"], ref[p + "d_v"])

    lead = load_mixer("l")
    load_attn = [local(ref[n], ref[n + "_v"]) for n in ("g2", "wq", "wk", "wf", "wv", "wg")]
    load_state = [local(ref[n], ref[n + "_v"]) for n in ("st", "eld", "hng")]
    load_out = local(ref["wo"], ref["wo_v"])
    load_g3 = local(ref["g3"], ref["g3_v"])
    trail = load_mixer("t")

    barrier = pltpu.get_barrier_semaphore()
    for o in range(1, R):
        pl.semaphore_signal(barrier, inc=1, device_id=row_peer(o)[1], device_id_type=MESH)
    for o in kv_order:
        pl.semaphore_signal(barrier, inc=1, device_id=kv_peer(o)[1], device_id_type=MESH)
    pl.semaphore_wait(barrier, R - 1 + K - 1)

    def gather_rows(buf):
        sems = group()
        for o in range(1, R):
            remote(buf.at[r], buf.at[r], row_peer(o)[1], sems)
        pending.append((buf.at[pl.ds(0, R - 1)], sems))
        return sems

    def flat(block):
        if hm % 16 == 0:
            return block.reshape(rows, -1)
        return block.astype(F32).reshape(rows, -1).astype(BF16)

    def normalised(s, buf, gain):
        wide = buf[...].astype(F32).reshape(rows, d)
        squares = jnp.sum(wide * wide, axis=1, keepdims=True)
        ref["scaled", s][...] = (wide * gain[...]).astype(BF16)
        return jnp.broadcast_to(squares, (rows, LANES)).reshape(K, hm, LANES)

    def row_scale(total):
        return lax.rsqrt(total / D + epsilon)[:, :1]

    def part(buf, i, a, b):
        return buf.at[i] if b - a == F else buf.at[i, :, :, pl.ds(a, b - a)]

    def piece(buf, i, a, b):
        return buf.at[i] if b - a == F else buf.at[i, :, pl.ds(a, b - a)]

    def send_squares(p, s, buf, gain):
        ss_send, ss_recv = ref[p, "ss_send", s], ref[p, "ss_recv", s]
        ss_send[...] = normalised(s, buf, gain)
        return to_kv_peers(
            lambda t: ss_send.at[t], lambda o: ss_recv.at[o - 1], ss_send.at[pl.ds(0, K - 1)]
        )

    def total_scale(p, s, sems):
        arrived(ref[p, "ss_recv", s], sems)
        total = ref[p, "ss_send", s][k]
        for o in kv_order:
            total = total + ref[p, "ss_recv", s][o - 1]
        return row_scale(total)

    def mixer_direct(p, s, buf, gain, loads):
        gu_loads, down_load = loads
        gu_send, gu_recv, h_all = ref[p, "gu_send", s], ref[p, "gu_recv", s], ref[p, "h_all", s]
        loaded(load_g1, load_g3)
        ss_sems = send_squares(p, s, buf, gain)
        gu_sems = []
        for (a, b), pair in zip(fspans, gu_loads):
            for i, name in enumerate("gu"):
                loaded(pair[i])
                product = jnp.dot(
                    ref["scaled", s][...], ref[p + name + "_v"][:, a:b], preferred_element_type=F32
                )
                gu_send[:, i, :, a:b] = product.reshape(K, hm, b - a).astype(BF16)
            gu_sems.append(
                to_kv_peers(
                    lambda t: part(gu_send, t, a, b),
                    lambda o: part(gu_recv, o - 1, a, b),
                    part(gu_send, pl.ds(0, K - 1), a, b),
                )
            )
        scale = total_scale(p, s, ss_sems)
        h_sems = []
        for (a, b), sems in zip(fspans, gu_sems):
            arrived(part(gu_recv, pl.ds(0, K - 1), a, b), sems)
            gate = gu_send[k, 0, :, a:b].astype(F32)
            up = gu_send[k, 1, :, a:b].astype(F32)
            for o in kv_order:
                gate = gate + gu_recv[o - 1, 0, :, a:b].astype(F32)
                up = up + gu_recv[o - 1, 1, :, a:b].astype(F32)
            h_all[k, :, a:b] = (silu(scale * gate) * (scale * up)).astype(BF16)
            mine = piece(h_all, k, a, b)
            h_sems.append(
                to_kv_peers(lambda t: mine, lambda o: mine, piece(h_all, pl.ds(0, K - 1), a, b))
            )
        loaded(down_load)
        acc = None
        for (a, b), sems in zip(fspans, h_sems):
            arrived(piece(h_all, pl.ds(0, K - 1), a, b), sems)
            product = jnp.dot(
                flat(h_all[:, :, a:b]), ref[p + "d_v"][a:b, :], preferred_element_type=F32
            )
            acc = product if acc is None else acc + product
        return acc
        yield

    def mixer_paired(p, s, buf, gain, loads):
        gu_loads, down_load = loads
        gu_f, gu_send, gu_recv = ref["gu_f", s], ref[p, "gu_send", s], ref[p, "gu_recv", s]
        relay, h_all = ref[p, "relay", s], ref[p, "h_all", s]
        loaded(load_g1 if p == "l" else load_g3)
        ss_sems = send_squares(p, s, buf, gain)
        sums, relays, hiddens = [], [], [None] * len(fspans)
        relayed, forwarded = RELAYED_SUMS[s], RELAYED_HIDDEN[s]

        def to_partner(c):
            a, b = fspans[c]
            remote(part(gu_send, partner, a, b), part(gu_recv, 0, a, b), {"kv": partner}, sums[c])
            pending.append((part(gu_send, pl.ds(0, 3), a, b), sums[c]))

        for c, ((a, b), pair) in enumerate(zip(fspans, gu_loads)):
            if c:
                yield
            for i, name in enumerate("gu"):
                loaded(pair[i])
                product = jnp.dot(
                    ref["scaled", s][...], ref[p + name + "_v"][:, a:b], preferred_element_type=F32
                ).reshape(K, hm, b - a)
                gu_f[:, i, :, a:b] = product
                gu_send[:, i, :, a:b] = product.astype(BF16)
            sums.append(group())
            if c < relayed:
                relays.append(arrival())
                cut = (pl.ds(across, 2), slice(None), slice(None), pl.ds(a, b - a))
                where = (slice(None), slice(None), slice(None), pl.ds(a, b - a))
                copy = described(
                    gu_send.at[cut], relay.at[where], {"kv": partner}, (sums[c][0], relays[c])
                )
                pl.when(outer)(copy.start)
            else:
                for t in (far, near):
                    remote(
                        part(gu_send, t, a, b), part(gu_recv, slot, a, b), {"kv": t}, sums[c]
                    )
            if c:
                to_partner(c - 1)
        to_partner(len(fspans) - 1)

        def pass_on(c):
            a, b = fspans[c]
            where = (slice(None), slice(None), slice(None), pl.ds(a, b - a))
            onward = [
                described(part(gu_send, t, a, b), part(gu_recv, 1, a, b), {"kv": t}, sums[c])
                for t in (far, near)
            ]

            @pl.when(inner)
            def _():
                arrived(relay.at[where], (0, relays[c]))
                both = gu_f[pl.ds(across, 2), :, :, a:b] + relay[:, :, :, a:b].astype(F32)
                gu_send[pl.ds(across, 2), :, :, a:b] = both.astype(BF16)
                for copy in onward:
                    copy.start()

        for c in range(relayed):
            yield
            pass_on(c)
        yield
        scale = total_scale(p, s, ss_sems)
        for c, (a, b) in enumerate(fspans):
            if c:
                yield
            gate, up = gu_f[k, 0, :, a:b], gu_f[k, 1, :, a:b]
            blocks = 2 if c < relayed else 3
            arrived(part(gu_recv, pl.ds(0, blocks), a, b), sums[c])
            for i in range(blocks):
                gate = gate + gu_recv[i, 0, :, a:b].astype(F32)
                up = up + gu_recv[i, 1, :, a:b].astype(F32)
            h_all[k, :, a:b] = (silu(scale * gate) * (scale * up)).astype(BF16)
            mine = h_all.at[k, :, pl.ds(a, b - a)]
            hiddens[c] = group()
            for t in (near, partner) if c in forwarded else (far, near, partner):
                remote(mine, mine, {"kv": t}, hiddens[c])
            if c in forwarded:
                inner_pending.append((h_all.at[:, :, pl.ds(a, b - a)], hiddens[c]))
                outer_pending.append((h_all.at[pl.ds(0, 2), :, pl.ds(a, b - a)], hiddens[c]))
            else:
                pending.append((h_all.at[pl.ds(0, 3), :, pl.ds(a, b - a)], hiddens[c]))
        for c in forwarded:
            yield
            a, b = fspans[c]
            blocks = [h_all.at[i, :, pl.ds(a, b - a)] for i in (near, far)]
            copies = [described(block, block, {"kv": partner}, hiddens[c]) for block in blocks]

            @pl.when(inner)
            def _():
                arrived(h_all.at[pl.ds(0, 3), :, pl.ds(a, b - a)], hiddens[c])
                for copy in copies:
                    copy.start()

        acc = None
        for c, (a, b) in enumerate(fspans):
            yield
            loaded(down_load)
            if c in forwarded:

                @pl.when(outer)
                def _():
                    arrived(h_all.at[pl.ds(0, 3), :, pl.ds(a, b - a)], hiddens[c])

            else:
                arrived(h_all.at[pl.ds(0, 3), :, pl.ds(a, b - a)], hiddens[c])
            product = jnp.dot(
                flat(h_all[:, :, a:b]), ref[p + "d_v"][a:b, :], preferred_element_type=F32
            )
            acc = product if acc is None else acc + product
        return acc

    mixer = mixer_paired if paired else mixer_direct

    def scatter_rows(p, s, value):
        send, recv = ref[p, "_send", s], ref[p, "_recv", s]
        send[...] = value.reshape(R, hr, d).astype(BF16)
        sems = group()
        for o in range(1, R):
            t, device = row_peer(o)
            remote(send.at[t], recv.at[o - 1], device, sems)
        pending.append((send.at[pl.ds(0, R - 1)], sems))
        return sems

    def scattered(p, s, sems):
        send, recv = ref[p, "_send", s], ref[p, "_recv", s]
        arrived(recv, sems)
        total = send[r].astype(F32)
        for o in range(1, R):
            total = total + recv[o - 1].astype(F32)
        return total

    def reduce_rows_twice(p, s, value, buf, factor, out):
        total = scattered(p, s, scatter_rows(p, s, value))
        out[r] = (buf[r].astype(F32) + factor * total).astype(BF16)
        arrived(out.at[pl.ds(0, R - 1)], gather_rows(out))
        return
        yield

    def reduce_rows_once(p, s, value, buf, factor, out):
        whole, send, recv, parts = ref["rows_f", s], ref[p, "_send", s], ref[p, "_recv", s], ref[p, "_parts", s]
        whole[...] = value.reshape(DP, TP, hr, d)
        first, second = group(), group()
        halves = [first[1]]
        spans_d = spans(d, 1)
        for a, b in spans_d:
            send[:, :, a:b] = whole[:, 1 - tp_i, :, a:b].astype(BF16)
            cut = (slice(None), slice(None), pl.ds(a, b - a))
            remote(send.at[cut], recv.at[cut], {"tp": 1 - tp_i}, (first[0], halves[a > 0]))
        pending.append((send, first))
        for (a, b), half in zip(spans_d, halves):
            yield
            arrived(recv.at[:, :, pl.ds(a, b - a)], (0, half))
            chip = whole[:, tp_i, :, a:b] + recv[:, :, a:b].astype(F32)
            parts[r, :, :, a:b] = chip.astype(BF16)
            mine = parts.at[r, :, :, pl.ds(a, b - a)]
            for o in sorted(range(1, R), key=lambda o: o % TP == 0):
                remote(mine, mine, row_peer(o)[1], second)
        pending.append((parts.at[pl.ds(0, R - 1)], second))
        yield
        arrived(parts.at[pl.ds(0, R - 1)], second)
        for j in range(DP):
            for c in range(TP):
                total = parts[c, j].astype(F32)
                for x in range(1, DP):
                    total = total + parts[x * TP + c, j].astype(F32)
                i = j * TP + c
                out[i] = (buf[i].astype(F32) + factor * total).astype(BF16)

    reduce_rows = reduce_rows_once if DP == 2 and TP == 2 else reduce_rows_twice

    def chain(s):
        x_all, a_all, s_all = ref["x_all", s], ref["a_all", s], ref["s_all", s]
        loaded(own_x[s])
        sems = gather_rows(x_all)
        yield
        arrived(x_all.at[pl.ds(0, R - 1)], sems)
        mixed = yield from mixer("l", s, x_all, ref["g1_v"], lead)
        yield from reduce_rows("p1", s, mixed, x_all, 0.5, a_all)

        loaded(*load_attn)
        squares = normalised(s, a_all, ref["g2_v"])
        f_send, f_recv = ref["f_send", s], ref["f_recv", s]
        q_send, q_recv = ref["q_send", s], ref["q_recv", s]
        v_send, v_recv = ref["v_send", s], ref["v_recv", s]

        def project(name, width):
            return jnp.dot(
                ref["scaled", s][...], ref[name + "_v"][...], preferred_element_type=F32
            ).reshape(K, hm, width)

        f_send[:, :, Wp:] = squares
        f_send[:, :, :W] = project("wf", W)

        def exchange(send, recv):
            return to_kv_peers(
                lambda t: send.at[t], lambda o: recv.at[o - 1], send.at[pl.ds(0, K - 1)]
            )

        f_sems = exchange(f_send, f_recv)
        q_send[:, 0, :, :W] = project("wq", W).astype(BF16)
        q_send[:, 1, :, :W] = project("wk", W).astype(BF16)
        q_sems = exchange(q_send, q_recv)
        v_send[:, 0] = project("wv", V).astype(BF16)
        v_send[:, 1] = project("wg", V).astype(BF16)
        v_sems = exchange(v_send, v_recv)
        yield
        loaded(*load_state)
        arrived(f_recv, f_sems)
        forget = f_send[k]
        for o in kv_order:
            forget = forget + f_recv[o - 1]
        scale = row_scale(forget[:, Wp:])
        forget = scale * forget[:, :W]
        mine = slice(s * hm, (s + 1) * hm)
        decay = jnp.exp(
            (jnp.minimum(forget, 0.0) - jnp.log1p(jnp.exp(-jnp.abs(forget)))) / 16.0
            + ref["eld_v"][mine]
        )
        columns, read, vals = ref["columns", s], ref["read", s], ref["vals", s]
        columns[0] = decay.T
        yield
        arrived(q_recv, q_sems)
        pair = []
        for i in range(2):
            total = q_send[k, i, :, :W].astype(F32)
            for o in kv_order:
                total = total + q_recv[o - 1, i, :, :W].astype(F32)
            pair.append(scale * total)
        queries = pair[0] * KEY_CHANNELS ** (-0.5)
        columns[1] = pair[1].T
        columns[2] = (queries * decay).T
        overlap = queries * pair[1]
        for b in range(hm):
            for h in range(heads):
                keys = slice(h * KEY_CHANNELS, (h + 1) * KEY_CHANNELS)
                lanes = slice(h * VALUE_DIM, (h + 1) * VALUE_DIM)
                read[b : b + 1, lanes] = jnp.sum(
                    columns[2, keys, b : b + 1] * ref["st_v"][s * hm + b, h], axis=0, keepdims=True
                )
        yield
        arrived(v_recv, v_sems)
        pair = []
        for i in range(2):
            total = v_send[k, i].astype(F32)
            for o in kv_order:
                total = total + v_recv[o - 1, i].astype(F32)
            pair.append(scale * total)
        vals[...] = pair[0]
        gates = silu(pair[1])
        hr_all = ref["hr_all", s]
        for h in range(heads):
            lanes = slice(h * VALUE_DIM, (h + 1) * VALUE_DIM)
            keys = slice(h * KEY_CHANNELS, (h + 1) * KEY_CHANNELS)
            out = read[:, lanes] + (
                jnp.sum(overlap[:, keys], axis=1, keepdims=True) * pair[0][:, lanes]
            )
            out = out * lax.rsqrt(jnp.mean(out * out, axis=1, keepdims=True) + epsilon)
            hr_all[k, :, lanes] = (out * ref["hng_v"][...] * gates[:, lanes]).astype(BF16)
        hr_sems = to_kv_peers(
            lambda t: hr_all.at[k], lambda o: hr_all.at[k], hr_all.at[pl.ds(0, K - 1)]
        )
        yield
        for b in range(hm):
            for h in range(heads):
                keys = slice(h * KEY_CHANNELS, (h + 1) * KEY_CHANNELS)
                lanes = slice(h * VALUE_DIM, (h + 1) * VALUE_DIM)
                ref["new_state"][s * hm + b, h] = (
                    columns[0, keys, b : b + 1] * ref["st_v"][s * hm + b, h]
                    + columns[1, keys, b : b + 1] * vals[b : b + 1, lanes]
                )
        yield
        loaded(load_out)
        arrived(hr_all.at[pl.ds(0, K - 1)], hr_sems)
        mixed = jnp.dot(flat(hr_all[...]), ref["wo_v"][...], preferred_element_type=F32)
        yield from reduce_rows("p2", s, mixed, a_all, 1.0, s_all)

        mixed = yield from mixer("t", s, s_all, ref["g3_v"], trail)
        sems = scatter_rows("p3", s, mixed)
        yield
        share = scattered("p3", s, sems)
        ref["result"][s * hr : (s + 1) * hr] = (s_all[r].astype(F32) + 0.5 * share).astype(BF16)

    chains = [chain(s) for s in range(S)]
    taken = {}
    for s, steps in enumerate(chains):
        next(steps)
        taken[s] = 0
    while taken:
        s = min(taken, key=lambda i: READY[i][taken[i]] if S > 1 else 0)
        if next(chains[s], chains) is chains:
            del taken[s]
        else:
            taken[s] += 1
    loaded(load_g3)
    for block, sems in pending:
        left(block, sems)
    if inner_pending:

        @pl.when(inner)
        def _():
            for block, sems in inner_pending:
                left(block, sems)

        @pl.when(outer)
        def _():
            for block, sems in outer_pending:
                left(block, sems)


ARGS = ("x", "st", "eld", "g1", "lg", "lu", "ld", "g2", "wq", "wk")
ARGS += ("wv", "wg", "wf", "hng", "wo", "g3", "tg", "tu", "td")


def store(result, state, result_out, state_out, sem):
    copies = [
        pltpu.make_async_copy(state, state_out, sem.at[0]),
        pltpu.make_async_copy(result, result_out, sem.at[1]),
    ]
    for copy in copies:
        copy.start()
    for copy in copies:
        copy.wait()


def per_device(sizes, *arrays):
    dp, tp, K = sizes
    R = dp * tp
    ref = dict(zip(ARGS, arrays))
    for n in ("g1", "g2", "g3", "hng"):
        ref[n] = ref[n].reshape(1, -1)
    mr, d = ref["x"].shape
    B, D = mr * R, d * K
    F = ref["lg"].shape[1]
    W, V = ref["wq"].shape[1], ref["wv"].shape[1]
    heads = W // KEY_CHANNELS
    Wp = padded(W)
    paired = K == PAIRS
    S = 2 if paired and mr * K == B and mr % 16 == 0 else 1
    rows, hr, hm = B // S, mr // S, B // K // S
    dims = (R, K, tp, D, B, d, F, W, V, heads, S)
    once = dp == 2 and tp == 2
    vm = {}
    for n in ARGS:
        if n != "x":
            vm[n + "_v"] = (ref[n].shape, ref[n].dtype)
    for s in range(S):
        for n in ("x_all", "a_all", "s_all"):
            vm[n, s] = ((R, hr, d), BF16)
        vm["scaled", s] = ((rows, d), BF16)
        for p in ("l", "t"):
            vm[p, "gu_send", s] = ((K, 2, hm, F), BF16)
            vm[p, "gu_recv", s] = ((K - 1, 2, hm, F), BF16)
            vm[p, "ss_send", s] = ((K, hm, LANES), F32)
            vm[p, "ss_recv", s] = ((K - 1, hm, LANES), F32)
            vm[p, "h_all", s] = ((K, hm, F), BF16)
            if paired:
                vm[p, "relay", s] = ((2, 2, hm, F), BF16)
        if paired:
            vm["gu_f", s] = ((K, 2, hm, F), F32)
        if once:
            vm["rows_f", s] = ((dp, tp, hr, d), F32)
        for p in ("p1", "p2", "p3"):
            if once and p != "p3":
                vm[p, "_send", s] = ((dp, hr, d), BF16)
                vm[p, "_recv", s] = ((dp, hr, d), BF16)
                vm[p, "_parts", s] = ((R, dp, hr, d), BF16)
            else:
                vm[p, "_send", s] = ((R, hr, d), BF16)
                vm[p, "_recv", s] = ((R - 1, hr, d), BF16)
        vm["f_send", s] = ((K, hm, Wp + LANES), F32)
        vm["f_recv", s] = ((K - 1, hm, Wp + LANES), F32)
        vm["q_send", s] = ((K, 2, hm, Wp), BF16)
        vm["q_recv", s] = ((K - 1, 2, hm, Wp), BF16)
        vm["v_send", s] = ((K, 2, hm, V), BF16)
        vm["v_recv", s] = ((K - 1, 2, hm, V), BF16)
        vm["columns", s] = ((3, W, hm), F32)
        vm["vals", s] = ((hm, V), F32)
        vm["read", s] = ((hm, V), F32)
        vm["hr_all", s] = ((K, hm, V), BF16)
    names = [*ARGS, "result", "new_state", *vm, "local_sem", "send_sem", "recv_sem"]
    chunks = len(SHARES) if paired else CHUNKS
    sems = S * (14 + 2 * (1 + 2 * chunks + max(RELAYED_SUMS)))
    outputs = pl.pallas_call(
        functools.partial(kernel, dims, names),
        out_shape=(
            pltpu.VMEM((mr, d), BF16),
            pltpu.VMEM(ref["st"].shape, F32),
        ),
        in_specs=[pl.BlockSpec(memory_space=pl.ANY)] * len(ARGS),
        out_specs=[pl.BlockSpec(memory_space=pltpu.VMEM)] * 2,
        scratch_shapes=[
            *[pltpu.VMEM(shape, dtype) for shape, dtype in vm.values()],
            pltpu.SemaphoreType.DMA((15 + S + 4 * chunks,)),
            pltpu.SemaphoreType.DMA((sems,)),
            pltpu.SemaphoreType.DMA((sems,)),
        ],
        compiler_params=pltpu.CompilerParams(
            collective_id=0, has_side_effects=True, vmem_limit_bytes=56 * 1024 * 1024
        ),
    )(*[ref[n] for n in ARGS])
    return pl.pallas_call(
        store,
        out_shape=(
            jax.ShapeDtypeStruct((mr, d), BF16),
            jax.ShapeDtypeStruct(ref["st"].shape, F32),
        ),
        in_specs=[pl.BlockSpec(memory_space=pltpu.VMEM)] * 2,
        out_specs=[pl.BlockSpec(memory_space=pl.ANY)] * 2,
        scratch_shapes=[pltpu.SemaphoreType.DMA((2,))],
    )(*[pltpu.with_memory_space_constraint(v, pltpu.VMEM) for v in outputs])


def solution(mesh):
    sizes = (mesh.shape["dp"], mesh.shape["tp"], mesh.shape["kv"])
    return jax.shard_map(
        functools.partial(per_device, sizes),
        mesh=mesh,
        in_specs=(
            P(("grp", "dp", "tp"), "kv"),
            P(("grp", "kv"), ("dp", "tp"), None, None),
            P(("grp", "kv"), ("dp", "tp")),
            P("kv"),
            P("kv", ("dp", "tp")),
            P("kv", ("dp", "tp")),
            P(("dp", "tp"), "kv"),
            P("kv"),
            P("kv", ("dp", "tp")),
            P("kv", ("dp", "tp")),
            P("kv", ("dp", "tp")),
            P("kv", ("dp", "tp")),
            P("kv", ("dp", "tp")),
            P(),
            P(("dp", "tp"), "kv"),
            P("kv"),
            P("kv", ("dp", "tp")),
            P("kv", ("dp", "tp")),
            P(("dp", "tp"), "kv"),
        ),
        out_specs=(P(("grp", "dp", "tp"), "kv"), P(("grp", "kv"), ("dp", "tp"), None, None)),
        check_vma=False,
    )
```
